32 devices in a mesh: sp: 8 (over z, y), tp: 4 (over x, core).
Axes of the slice: x: 2, y: 2, z: 4, core: 2. Of those that a mesh axis runs over, the one named last changes fastest.
Arguments:
- stream_in: bfloat16 [4096, 4096], P('sp', 'tp'), may hold values from -12 to 12
- norm_gain: float32 [2, 4096], replicated, may hold values from 0.1 to 1.9
- value_proj: bfloat16 [2, 4096, 4096], P(None, 'sp', 'tp'), may hold values from -0.09375 to 0.09375
- gate_proj: bfloat16 [2, 4096, 4096], P(None, 'sp', 'tp'), may hold values from -0.09375 to 0.09375
- out_proj: bfloat16 [2, 4096, 4096], P(None, 'sp', 'tp'), may hold values from -0.1875 to 0.1875
- conv_taps: float32 [2, 4, 4096], replicated, may hold values from -3 to 3
- block_gates: bfloat16 [2, 2, 2, 4096, 128], P(None, None, None, 'tp'), may hold values from -0.5 to 0.5
- forget_rate: float32 [2, 2, 4096], replicated, may hold values from 0 to 0.05, as said below
Outputs:
- stream_out: bfloat16 [4096, 4096], P('sp', 'tp')
The draws below stay inside these ranges and needn't reach their ends.
Inputs may be any that keep to these rules, and one draw needn't show every extreme that they name: `forget_rate`: positive.
All inputs are finite; a program needn't handle non-finite values.
Results may differ from the reference program's by a relative error of at most 0.025.
Values may be sent and summed in bfloat16 or wider, within the bound.
A program may use at most 192 MiB of HBM per device.

```python
import math
import jax
import jax.numpy as jnp
from jax import lax

D = 4096
W = 4096
BLK = 128
LAYERS = 2
TOK_DEV = 512
TOKENS = 4096
N_TP = 4


def draw_stream_in(key, part):
    subkeys = jax.random.split(key, 6)
    base = jax.random.normal(subkeys[0], (TOKENS, D), jnp.float32)
    phase = jax.random.uniform(subkeys[1], (), jnp.float32, -math.pi, math.pi)
    position = jnp.arange(D).astype(jnp.float32) / D
    channel_scale = jnp.exp(0.9 * jnp.cos(2.0 * math.pi * position + phase) + jax.random.uniform(subkeys[2], (D,), jnp.float32, -0.3, 0.3))
    nblocks = (TOKENS + TOK_DEV - 1) // TOK_DEV
    block_mix = jax.random.normal(subkeys[3], (nblocks, D), jnp.float32)
    block_mix = block_mix * jax.random.uniform(subkeys[4], (nblocks, 1), jnp.float32, 0.5, 3.0)
    row_block = jnp.arange(TOKENS) // TOK_DEV
    result = base * channel_scale + block_mix[row_block]
    return jnp.clip(result, -12.0, 12.0).astype(jnp.bfloat16)


def draw_forget_rate(key, part):
    subkeys = jax.random.split(key, 3)
    shape = (LAYERS, 2, W)
    keep_share = 0.5
    slow_pick = jax.random.uniform(subkeys[0], shape, jnp.float32) < keep_share
    slow_rate = jnp.exp(jax.random.uniform(subkeys[1], shape, jnp.float32, math.log(0.02), math.log(0.2))) / TOKENS
    fast_hi = max(0.012, 0.4 / TOK_DEV)
    fast_rate = jnp.exp(jax.random.uniform(subkeys[2], shape, jnp.float32, math.log(fast_hi / 4.0), math.log(fast_hi)))
    return jnp.where(slow_pick, slow_rate, fast_rate)


def block_levels(stream_key, extent, shards, smallest, top_value):
    level, own = 1.0, jax.random.fold_in(stream_key, 6)
    for dim, blocks in shards:
        draws = jnp.exp(jax.random.uniform(jax.random.fold_in(own, dim), (blocks,), jnp.float32, smallest / len(shards), top_value / len(shards)))
        level = level * jnp.repeat(draws, extent[dim] // blocks).reshape([-1 if axis == dim else 1 for axis in range(len(extent))])
    return level


def scatter_about(own_key, dims, scale, reach, pieces=(), kind=jnp.bfloat16):
    level = block_levels(own_key, dims, pieces, -0.22, 0.18) if pieces else 1.0
    array = jax.random.normal(own_key, dims, jnp.float32) * scale * level
    return jnp.minimum(jnp.maximum(array, -reach), reach).astype(kind)


def setup_inputs(seed: int = 0) -> dict:
    seeds = jax.random.split(jax.random.key(seed), 9)
    stream_in = draw_stream_in(jax.random.fold_in(seeds[8], 71), 0)
    norm_gain = jnp.clip(1.0 + 0.18 * jax.random.normal(seeds[1], (LAYERS, D), jnp.float32), 0.1, 1.9)
    value_proj = scatter_about(seeds[2], (LAYERS, D, W), D ** -0.5, 0.09375, ((1, 8), (2, 4)))
    gate_proj = scatter_about(seeds[3], (LAYERS, D, W), D ** -0.5, 0.09375, ((1, 8), (2, 4)))
    out_proj = scatter_about(seeds[4], (LAYERS, D, W), (W // 4) ** -0.5, 0.1875, ((1, 8), (2, 4)))
    conv_taps = scatter_about(seeds[5], (LAYERS, 4, W), 0.8, 3.0, (), jnp.float32)
    block_gates = scatter_about(seeds[6], (LAYERS, 2, 2, W, BLK), BLK ** -0.5, 0.5, ((3, 4),))
    forget_rate = draw_forget_rate(jax.random.fold_in(seeds[8], 71), 0)
    return dict(stream_in=stream_in, norm_gain=norm_gain, value_proj=value_proj, gate_proj=gate_proj, out_proj=out_proj, conv_taps=conv_taps, block_gates=block_gates, forget_rate=forget_rate)


GATE_SCALE = 8.0
NORM_EPS = 1e-06

def pair_combine(earlier, latter):
    return (earlier[0] * latter[0], latter[0] * earlier[1] + latter[1])

def convolve(padded, taps_layer, length):
    values = padded.astype(jnp.float32)
    return sum((values[offset:offset + length] * taps_layer[offset] for offset in range(4)))

def gate_inputs(conv_out, gate_layer):
    count, width = conv_out.shape
    block_size = gate_layer.shape[-1]
    nblocks = width // block_size
    blocked = conv_out.reshape(count, nblocks, block_size)
    weights = gate_layer.astype(jnp.float32).reshape(4, nblocks, block_size, block_size)
    pre = jnp.einsum('tnc,gncd->gtnd', blocked, weights, precision=lax.Precision.HIGHEST)
    return pre.reshape(4, count, width)

def decay_inputs(conv_out, pre, rate_layer, direction):
    recur_gate = jax.nn.sigmoid(pre[2 * direction])
    input_gate = jax.nn.sigmoid(pre[2 * direction + 1])
    log_decay = -GATE_SCALE * recur_gate * rate_layer[direction]
    decay = jnp.exp(log_decay)
    drive = jnp.sqrt(-jnp.expm1(2.0 * log_decay)) * input_gate * conv_out
    return (decay, drive)

def reference(stream_in, norm_gain, value_proj, gate_proj, out_proj, conv_taps, block_gates, forget_rate):
    stream = stream_in
    length = stream_in.shape[0]
    group_width = W // N_TP
    for layer_index in range(LAYERS):
        values = stream.astype(jnp.float32)
        scale = lax.rsqrt(lax.optimization_barrier(jnp.mean(values * values, axis=1, keepdims=True)) + NORM_EPS)
        normed = (values * scale * norm_gain[layer_index]).astype(jnp.bfloat16)
        mix_in = jnp.dot(normed, value_proj[layer_index], preferred_element_type=jnp.float32).astype(jnp.bfloat16)
        gate_z = jnp.dot(normed, gate_proj[layer_index], preferred_element_type=jnp.float32).astype(jnp.bfloat16)
        padded = jnp.pad(mix_in, ((2, 1), (0, 0)))
        conv_out = convolve(padded, conv_taps[layer_index], length)
        pre = gate_inputs(conv_out, block_gates[layer_index])
        fwd_decay, fwd_drive = decay_inputs(conv_out, pre, forget_rate[layer_index], 0)
        bwd_decay, bwd_drive = decay_inputs(conv_out, pre, forget_rate[layer_index], 1)
        _, fwd_state = lax.associative_scan(pair_combine, (fwd_decay, fwd_drive), axis=0)
        _, bwd_flip = lax.associative_scan(pair_combine, (jnp.flip(bwd_decay, 0), jnp.flip(bwd_drive, 0)), axis=0)
        both = fwd_state + jnp.flip(bwd_flip, 0)
        mixed = (both * jax.nn.silu(gate_z.astype(jnp.float32))).astype(jnp.bfloat16)
        branch = jnp.zeros((length, D), jnp.float32)
        for group in range(N_TP):
            part = lax.dot_general(mixed[:, group * group_width:(group + 1) * group_width], out_proj[layer_index][:, group * group_width:(group + 1) * group_width], (((1,), (1,)), ((), ())), preferred_element_type=jnp.float32)
            rounded = lax.optimization_barrier(part.astype(jnp.bfloat16))
            branch = branch + rounded.astype(jnp.float32)
        stream = (values + branch).astype(jnp.bfloat16)
    return stream
```

```python
import jax
import jax.numpy as jnp
from jax import lax
from jax.experimental import pallas as pl
from jax.experimental.pallas import tpu as pltpu
from jax.sharding import PartitionSpec as P

GATE_SCALE = 8.0
NORM_EPS = 1e-06
ROW_STEPS = 4
CHUNKS = 8


def solve_gates(pre_r, pre_i, rate, conv):
    recur_gate = jax.nn.sigmoid(pre_r)
    input_gate = jax.nn.sigmoid(pre_i)
    log_decay = -GATE_SCALE * recur_gate * rate
    decay = jnp.exp(log_decay)
    twice = 2.0 * log_decay
    series = jnp.ones_like(twice)
    for order in range(10, 1, -1):
        series = 1.0 + twice * (1.0 / order) * series
    loss = jnp.where(twice > -0.9, -twice * series, 1.0 - jnp.exp(twice))
    return decay, jnp.sqrt(loss) * input_gate * conv


def scan_kernel(
    mix_ref, before_ref, after_ref, taps_ref, gates_ref, rate_ref,
    both_ref, fcum_ref, bcum_ref, ends_ref,
    padded, fa, fu, ba, bu, fh, fp, bh, bp,
):
    count, width = mix_ref.shape
    padded[0:8, :] = before_ref[...].astype(jnp.float32)
    padded[8 : count + 8, :] = mix_ref[...].astype(jnp.float32)
    padded[count + 8 : count + 16, :] = after_ref[...].astype(jnp.float32)
    weights = jnp.concatenate([gates_ref[i] for i in range(4)], axis=1)
    rows = count // ROW_STEPS
    for step in range(ROW_STEPS):
        base = step * rows
        conv = padded[base + 6 : base + 6 + rows, :] * taps_ref[0:1, :]
        for tap in range(1, 4):
            conv += padded[base + 6 + tap : base + 6 + tap + rows, :] * taps_ref[tap : tap + 1, :]
        high = conv.astype(jnp.bfloat16)
        low = (conv - high.astype(jnp.float32)).astype(jnp.bfloat16)
        pre = jnp.dot(high, weights, preferred_element_type=jnp.float32)
        pre += jnp.dot(low, weights, preferred_element_type=jnp.float32)
        for e, (decay_to, drive_to) in enumerate(((fa, fu), (ba, bu))):
            decay, drive = solve_gates(
                pre[:, 2 * e * width : (2 * e + 1) * width],
                pre[:, (2 * e + 1) * width : (2 * e + 2) * width],
                rate_ref[e : e + 1, :],
                conv,
            )
            decay_to[base : base + rows, :] = decay
            drive_to[base : base + rows, :] = drive
    chunk = count // CHUNKS

    def advance(j, carry):
        f_state, f_prod, b_state, b_prod = carry
        at = pl.ds(j, CHUNKS, stride=chunk)
        back = pl.ds(chunk - 1 - j, CHUNKS, stride=chunk)
        f_decay, b_decay = fa[at, :], ba[back, :]
        f_state = f_decay * f_state + fu[at, :]
        f_prod = f_decay * f_prod
        b_state = b_decay * b_state + bu[back, :]
        b_prod = b_decay * b_prod
        fh[at, :] = f_state
        fp[at, :] = f_prod
        bh[back, :] = b_state
        bp[back, :] = b_prod
        return f_state, f_prod, b_state, b_prod

    zeros = jnp.zeros((CHUNKS, width), jnp.float32)
    ones = jnp.ones((CHUNKS, width), jnp.float32)
    f_state, f_prod, b_state, b_prod = lax.fori_loop(
        0, chunk, advance, (zeros, ones, zeros, ones), unroll=8
    )
    zero_row, one_row = zeros[0:1], ones[0:1]
    f_in, b_in = [], [None] * CHUNKS
    state, prod = zero_row, one_row
    for c in range(CHUNKS):
        f_in.append((state, prod))
        state = f_prod[c : c + 1] * state + f_state[c : c + 1]
        prod = f_prod[c : c + 1] * prod
    f_end, f_all = state, prod
    state, prod = zero_row, one_row
    for c in reversed(range(CHUNKS)):
        b_in[c] = (state, prod)
        state = b_prod[c : c + 1] * state + b_state[c : c + 1]
        prod = b_prod[c : c + 1] * prod
    ends_ref[...] = jnp.concatenate([f_all, f_end, prod, state, zeros[0:4]], axis=0)
    for c in range(CHUNKS):
        part = slice(c * chunk, (c + 1) * chunk)
        f_local, b_local = fp[part, :], bp[part, :]
        both_ref[part, :] = (
            fh[part, :] + f_local * f_in[c][0] + bh[part, :] + b_local * b_in[c][0]
        )
        fcum_ref[part, :] = f_local * f_in[c][1]
        bcum_ref[part, :] = b_local * b_in[c][1]


def local_scan(mix_in, before, after, taps_own, gates, rate_own):
    count, width = mix_in.shape
    block = gates.shape[-1]
    gates = gates.reshape(4, width, block)
    tile = pl.BlockSpec((count, block), lambda i: (0, i))
    edge = pl.BlockSpec((8, block), lambda i: (0, i))
    whole = jax.ShapeDtypeStruct((count, width), jnp.float32)
    slab = pltpu.VMEM((count, block), jnp.float32)
    return pl.pallas_call(
        scan_kernel,
        grid=(width // block,),
        in_specs=[
            tile,
            edge,
            edge,
            pl.BlockSpec((4, block), lambda i: (0, i)),
            pl.BlockSpec((4, block, block), lambda i: (0, i, 0)),
            pl.BlockSpec((2, block), lambda i: (0, i)),
        ],
        out_specs=[tile, tile, tile, edge],
        out_shape=[whole, whole, whole, jax.ShapeDtypeStruct((8, width), jnp.float32)],
        scratch_shapes=[pltpu.VMEM((count + 16, block), jnp.float32)] + [slab] * 8,
        cost_estimate=pl.CostEstimate(
            flops=count * width * 8000, bytes_accessed=count * width * 16, transcendentals=0
        ),
        name="local_scan",
    )(mix_in, before, after, taps_own, gates, rate_own)


def halo(cells):
    count = lax.axis_size("sp")
    ends = count - 1
    rows = cells.shape[0]
    before = lax.ppermute(cells[rows - 8 :], "sp", [(i, i + 1) for i in range(ends)])
    after = lax.ppermute(cells[:8], "sp", [(i + 1, i) for i in range(ends)])
    return before, after


def entering_states(ends):
    count = lax.axis_size("sp")
    rank = lax.axis_index("sp")
    came_from = [None]
    for k in range(1, count):
        came_from.append(
            lax.ppermute(ends, "sp", [(i, (i + k) % count) for i in range(count)])
        )
    forward = jnp.zeros_like(ends[0])
    backward = jnp.zeros_like(ends[0])
    for k in range(count - 1, 0, -1):
        peer = came_from[k]
        forward = jnp.where(k <= rank, peer[0] * forward + peer[1], forward)
    for k in range(count - 1, 0, -1):
        peer = came_from[count - k]
        backward = jnp.where(rank + k < count, peer[2] * backward + peer[3], backward)
    return forward, backward


def per_device(
    stream_in, norm_gain, value_proj, gate_proj, out_proj, conv_taps, block_gates, forget_rate
):
    tp_rank = lax.axis_index("tp")
    tokens_own = stream_in.shape[0]
    feat_own = stream_in.shape[1]
    width_own = value_proj.shape[2]
    stream = stream_in
    for layer_index in range(value_proj.shape[0]):
        full_x, full_z, full_out = (
            lax.all_gather(value_proj[layer_index], "sp", axis=0, tiled=True),
            lax.all_gather(gate_proj[layer_index], "sp", axis=0, tiled=True),
            lax.all_gather(out_proj[layer_index], "sp", axis=0, tiled=True),
        )
        values = stream.astype(jnp.float32)
        squares = lax.psum(jnp.sum(values * values, axis=1), "tp")
        scale = lax.rsqrt(squares / norm_gain.shape[1] + NORM_EPS)
        gain_own = lax.dynamic_slice_in_dim(norm_gain[layer_index], tp_rank * feat_own, feat_own, 0)
        normed = (values * scale[:, None] * gain_own).astype(jnp.bfloat16)
        piece = lax.all_gather(normed, "tp", axis=1, tiled=True)
        proj_x = jnp.dot(piece, full_x, preferred_element_type=jnp.float32)
        proj_z = jnp.dot(piece, full_z, preferred_element_type=jnp.float32)
        mix_in = proj_x.astype(jnp.bfloat16)
        gate_z = proj_z.astype(jnp.bfloat16)
        before, after = halo(mix_in)
        taps_own = lax.dynamic_slice_in_dim(
            conv_taps[layer_index], tp_rank * width_own, width_own, 1
        )
        rate_own = lax.dynamic_slice_in_dim(
            forget_rate[layer_index], tp_rank * width_own, width_own, 1
        )
        both, f_cum, b_cum, ends = local_scan(
            mix_in, before, after, taps_own, block_gates[layer_index], rate_own
        )
        enter, leave = entering_states(ends)
        both = both + f_cum * enter + b_cum * leave
        mixed = (both * jax.nn.silu(gate_z.astype(jnp.float32))).astype(jnp.bfloat16)
        partial_value = lax.dot_general(
            mixed, full_out, (((1,), (1,)), ((), ())), preferred_element_type=jnp.float32
        )
        branch = lax.psum_scatter(
            partial_value.astype(jnp.bfloat16), "tp", scatter_dimension=1, tiled=True
        ).astype(jnp.float32)
        stream = (values + branch).astype(jnp.bfloat16)
    return stream


def solution(mesh):
    placed = (
        P("sp", "tp"),
        P(),
        P(None, "sp", "tp"),
        P(None, "sp", "tp"),
        P(None, "sp", "tp"),
        P(),
        P(None, None, None, "tp", None),
        P(),
    )
    return jax.shard_map(
        per_device, mesh=mesh, in_specs=placed, out_specs=P("sp", "tp"), check_vma=False
    )
```

```python
import jax
import jax.numpy as jnp
from jax import lax
from jax.experimental import pallas as pl
from jax.experimental.pallas import tpu as pltpu
from jax.sharding import PartitionSpec as P

GATE_SCALE = 8.0
NORM_EPS = 1e-06
ROW_STEPS = 4
CHUNKS = 8


def solve_gates(pre_r, pre_i, rate, conv):
    recur_gate = jax.nn.sigmoid(pre_r)
    input_gate = jax.nn.sigmoid(pre_i)
    log_decay = -GATE_SCALE * recur_gate * rate
    decay = jnp.exp(log_decay)
    twice = 2.0 * log_decay
    series = jnp.ones_like(twice)
    for order in range(10, 1, -1):
        series = 1.0 + twice * (1.0 / order) * series
    loss = jnp.where(twice > -0.9, -twice * series, 1.0 - jnp.exp(twice))
    return decay, jnp.sqrt(loss) * input_gate * conv


def scan_kernel(
    mix_ref, before_ref, after_ref, taps_ref, gates_ref, rate_ref,
    both_ref, fcum_ref, bcum_ref, ends_ref,
    padded, fa, fu, ba, bu, fh, fp, bh, bp,
):
    count, width = mix_ref.shape
    padded[0:8, :] = before_ref[...].astype(jnp.float32)
    padded[8 : count + 8, :] = mix_ref[...].astype(jnp.float32)
    padded[count + 8 : count + 16, :] = after_ref[...].astype(jnp.float32)
    weights = jnp.concatenate([gates_ref[i] for i in range(4)], axis=1)
    rows = count // ROW_STEPS
    for step in range(ROW_STEPS):
        base = step * rows
        conv = padded[base + 6 : base + 6 + rows, :] * taps_ref[0:1, :]
        for tap in range(1, 4):
            conv += padded[base + 6 + tap : base + 6 + tap + rows, :] * taps_ref[tap : tap + 1, :]
        high = conv.astype(jnp.bfloat16)
        low = (conv - high.astype(jnp.float32)).astype(jnp.bfloat16)
        pre = jnp.dot(high, weights, preferred_element_type=jnp.float32)
        pre += jnp.dot(low, weights, preferred_element_type=jnp.float32)
        for e, (decay_to, drive_to) in enumerate(((fa, fu), (ba, bu))):
            decay, drive = solve_gates(
                pre[:, 2 * e * width : (2 * e + 1) * width],
                pre[:, (2 * e + 1) * width : (2 * e + 2) * width],
                rate_ref[e : e + 1, :],
                conv,
            )
            decay_to[base : base + rows, :] = decay
            drive_to[base : base + rows, :] = drive
    chunk = count // CHUNKS

    def advance(j, carry):
        f_state, f_prod, b_state, b_prod = carry
        at = pl.ds(j, CHUNKS, stride=chunk)
        back = pl.ds(chunk - 1 - j, CHUNKS, stride=chunk)
        f_decay, b_decay = fa[at, :], ba[back, :]
        f_state = f_decay * f_state + fu[at, :]
        f_prod = f_decay * f_prod
        b_state = b_decay * b_state + bu[back, :]
        b_prod = b_decay * b_prod
        fh[at, :] = f_state
        fp[at, :] = f_prod
        bh[back, :] = b_state
        bp[back, :] = b_prod
        return f_state, f_prod, b_state, b_prod

    zeros = jnp.zeros((CHUNKS, width), jnp.float32)
    ones = jnp.ones((CHUNKS, width), jnp.float32)
    f_state, f_prod, b_state, b_prod = lax.fori_loop(
        0, chunk, advance, (zeros, ones, zeros, ones), unroll=8
    )
    zero_row, one_row = zeros[0:1], ones[0:1]
    f_in, b_in = [], [None] * CHUNKS
    state, prod = zero_row, one_row
    for c in range(CHUNKS):
        f_in.append((state, prod))
        state = f_prod[c : c + 1] * state + f_state[c : c + 1]
        prod = f_prod[c : c + 1] * prod
    f_end, f_all = state, prod
    state, prod = zero_row, one_row
    for c in reversed(range(CHUNKS)):
        b_in[c] = (state, prod)
        state = b_prod[c : c + 1] * state + b_state[c : c + 1]
        prod = b_prod[c : c + 1] * prod
    ends_ref[...] = jnp.concatenate([f_all, f_end, prod, state, zeros[0:4]], axis=0)
    for c in range(CHUNKS):
        part = slice(c * chunk, (c + 1) * chunk)
        f_local, b_local = fp[part, :], bp[part, :]
        both_ref[part, :] = (
            fh[part, :] + f_local * f_in[c][0] + bh[part, :] + b_local * b_in[c][0]
        )
        fcum_ref[part, :] = f_local * f_in[c][1]
        bcum_ref[part, :] = b_local * b_in[c][1]


def local_scan(mix_in, before, after, taps_own, gates, rate_own):
    count, width = mix_in.shape
    block = gates.shape[-1]
    gates = gates.reshape(4, width, block)
    tile = pl.BlockSpec((count, block), lambda i: (0, i))
    edge = pl.BlockSpec((8, block), lambda i: (0, i))
    whole = jax.ShapeDtypeStruct((count, width), jnp.float32)
    slab = pltpu.VMEM((count, block), jnp.float32)
    return pl.pallas_call(
        scan_kernel,
        grid=(width // block,),
        in_specs=[
            tile,
            edge,
            edge,
            pl.BlockSpec((4, block), lambda i: (0, i)),
            pl.BlockSpec((4, block, block), lambda i: (0, i, 0)),
            pl.BlockSpec((2, block), lambda i: (0, i)),
        ],
        out_specs=[tile, tile, tile, edge],
        out_shape=[whole, whole, whole, jax.ShapeDtypeStruct((8, width), jnp.float32)],
        scratch_shapes=[pltpu.VMEM((count + 16, block), jnp.float32)] + [slab] * 8,
        cost_estimate=pl.CostEstimate(
            flops=count * width * 8000, bytes_accessed=count * width * 16, transcendentals=0
        ),
        name="local_scan",
    )(mix_in, before, after, taps_own, gates, rate_own)


def halo(cells):
    count = lax.axis_size("sp")
    ends = count - 1
    rows = cells.shape[0]
    before = lax.ppermute(cells[rows - 8 :], "sp", [(i, i + 1) for i in range(ends)])
    after = lax.ppermute(cells[:8], "sp", [(i + 1, i) for i in range(ends)])
    return before, after


def entering_states(ends):
    count = lax.axis_size("sp")
    rank = lax.axis_index("sp")
    came_from = [None]
    for k in range(1, count):
        came_from.append(
            lax.ppermute(ends, "sp", [(i, (i + k) % count) for i in range(count)])
        )
    forward = jnp.zeros_like(ends[0])
    backward = jnp.zeros_like(ends[0])
    for k in range(count - 1, 0, -1):
        peer = came_from[k]
        forward = jnp.where(k <= rank, peer[0] * forward + peer[1], forward)
    for k in range(count - 1, 0, -1):
        peer = came_from[count - k]
        backward = jnp.where(rank + k < count, peer[2] * backward + peer[3], backward)
    return forward, backward


def ring_rank(position, count):
    return jnp.where(
        position < (count + 1) // 2, 2 * position, 2 * (count - 1 - position) + 1
    )


def ring_gather(shards, gate):
    count = lax.axis_size("sp")
    rank = lax.axis_index("sp")
    position = jnp.where(rank % 2 == 0, rank // 2, count - 1 - rank // 2)
    order = list(range(0, count, 2)) + list(reversed(range(1, count, 2)))
    up = [(order[p], order[(p + 1) % count]) for p in range(count)]
    down = [(b, a) for a, b in up]
    if gate is not None:
        shards = lax.optimization_barrier((*shards, *gate))[: len(shards)]
    found = [[(rank, shard)] for shard in shards]
    above, below = list(shards), list(shards)
    steps = []
    far = count // 2
    for k in range(1, far + 1):
        moved = []
        for m in range(len(shards)):
            ups = far if m % 2 == 0 else count - 1 - far
            if k <= ups:
                above[m] = lax.ppermute(above[m], "sp", up)
                moved.append((m, above, ring_rank((position - k) % count, count)))
            if k <= count - 1 - ups:
                below[m] = lax.ppermute(below[m], "sp", down)
                moved.append((m, below, ring_rank((position + k) % count, count)))
        landed = lax.optimization_barrier(tuple(held[m] for m, held, _ in moved))
        for (m, held, owner), block in zip(moved, landed):
            held[m] = block
            found[m].append((owner, block))
        steps.append(landed)
    return found, steps


def after_step(value, steps, index):
    if steps is None or index >= len(steps):
        return value
    return lax.optimization_barrier((value, *steps[index]))[0]


def project(piece, found):
    total = None
    for owner, block in found:
        rows = block.shape[0]
        part = lax.dynamic_slice_in_dim(piece, owner * rows, rows, 1)
        term = jnp.dot(part, block, preferred_element_type=jnp.float32)
        total = term if total is None else total + term
    return total


def project_back(mixed, found, features):
    result = jnp.zeros((mixed.shape[0], features), jnp.bfloat16)
    for owner, block in found:
        term = lax.dot_general(
            mixed, block, (((1,), (1,)), ((), ())), preferred_element_type=jnp.float32
        )
        result = lax.dynamic_update_slice_in_dim(
            result, term.astype(jnp.bfloat16), owner * block.shape[0], 1
        )
    return result


def per_device(
    stream_in, norm_gain, value_proj, gate_proj, out_proj, conv_taps, block_gates, forget_rate
):
    tp_rank = lax.axis_index("tp")
    tokens_own = stream_in.shape[0]
    feat_own = stream_in.shape[1]
    width_own = value_proj.shape[2]
    stream = stream_in
    gate = None
    rings = []
    for layer_index in range(value_proj.shape[0]):
        in_found, in_steps = ring_gather(
            (value_proj[layer_index], gate_proj[layer_index]), gate
        )
        gate = in_steps[max(len(in_steps) - 2, 0)]
        out_found, out_steps = ring_gather((out_proj[layer_index],), gate)
        gate = out_steps[max(len(out_steps) - 2, 0)]
        rings.append((in_found, in_steps, out_found, out_steps))
    for layer_index in range(value_proj.shape[0]):
        (found_x, found_z), in_steps, (found_out,), out_steps = rings[layer_index]
        ahead = rings[layer_index + 1][1] if layer_index + 1 < len(rings) else None
        values = stream.astype(jnp.float32)
        squares = lax.psum(jnp.sum(values * values, axis=1), "tp")
        scale = lax.rsqrt(squares / norm_gain.shape[1] + NORM_EPS)
        gain_own = lax.dynamic_slice_in_dim(norm_gain[layer_index], tp_rank * feat_own, feat_own, 0)
        normed = (values * scale[:, None] * gain_own).astype(jnp.bfloat16)
        piece = lax.all_gather(normed, "tp", axis=1, tiled=True)
        piece = after_step(piece, in_steps, len(in_steps) - 2)
        proj_x = project(piece, found_x)
        proj_z = project(piece, found_z)
        mix_in = proj_x.astype(jnp.bfloat16)
        gate_z = proj_z.astype(jnp.bfloat16)
        mix_in = after_step(mix_in, out_steps, 0)
        before, after = halo(mix_in)
        taps_own = lax.dynamic_slice_in_dim(
            conv_taps[layer_index], tp_rank * width_own, width_own, 1
        )
        rate_own = lax.dynamic_slice_in_dim(
            forget_rate[layer_index], tp_rank * width_own, width_own, 1
        )
        both, f_cum, b_cum, ends = local_scan(
            mix_in, before, after, taps_own, block_gates[layer_index], rate_own
        )
        both = after_step(both, out_steps, 1)
        enter, leave = entering_states(ends)
        both = both + f_cum * enter + b_cum * leave
        mixed = (both * jax.nn.silu(gate_z.astype(jnp.float32))).astype(jnp.bfloat16)
        partial_value = project_back(mixed, found_out, norm_gain.shape[1])
        partial_value = after_step(partial_value, ahead, 0)
        branch = lax.psum_scatter(
            partial_value, "tp", scatter_dimension=1, tiled=True
        ).astype(jnp.float32)
        branch = after_step(branch, ahead, 1)
        stream = (values + branch).astype(jnp.bfloat16)
    return stream


def solution(mesh):
    placed = (
        P("sp", "tp"),
        P(),
        P(None, "sp", "tp"),
        P(None, "sp", "tp"),
        P(None, "sp", "tp"),
        P(),
        P(None, None, None, "tp", None),
        P(),
    )
    return jax.shard_map(
        per_device, mesh=mesh, in_specs=placed, out_specs=P("sp", "tp"), check_vma=False
    )
```
